512 devices in a mesh: sp: 16 (over z), fs: 4 (over y), tp: 8 (over x, core).
Axes of the slice: x: 4, y: 4, z: 16, core: 2. Of those that a mesh axis runs over, the one named last changes fastest.
Arguments:
- tokens: bfloat16 [8, 2048, 1024], P('tp', 'sp'), may hold values from -6 to 6
- in_gain: float32 [1024], replicated, may hold values from 0.1 to 1.9
- query_weight: bfloat16 [1024, 1024], P('sp', 'fs'), may hold values from -0.1875 to 0.1875
- key_weight: bfloat16 [1024, 256], P('sp', 'fs'), may hold values from -0.1875 to 0.1875
- value_weight: bfloat16 [1024, 256], P('sp', 'fs'), may hold values from -0.1875 to 0.1875
- attn_gate_weight: bfloat16 [1024, 1024], P('sp', 'fs'), may hold values from -0.1875 to 0.1875
- state_in_weight: bfloat16 [1024, 512], P('sp', 'fs'), may hold values from -0.1875 to 0.1875
- state_gate_weight: bfloat16 [1024, 512], P('sp', 'fs'), may hold values from -0.1875 to 0.1875
- sink_logits: float32 [16], P('fs'), may hold values from 2 to 6
- decay_rate: float32 [32, 64], P('fs'), may hold values from 0.05 to 1.5
- rotation: float32 [32, 64], P('fs'), may hold values from 0.3 to 1.5
- step_size: float32 [32], P('fs'), may hold values from 0.5 to 2
- input_real: float32 [32, 64, 16], P('fs'), may hold values from -1 to 1
- input_imag: float32 [32, 64, 16], P('fs'), may hold values from -1 to 1
- output_real: float32 [32, 16, 64], P('fs'), may hold values from -0.01171875 to 0.01171875
- output_imag: float32 [32, 16, 64], P('fs'), may hold values from -0.01171875 to 0.01171875
- skip_scale: float32 [512], P('fs'), may hold values from -4 to 4
- focus_result_coefficients: bfloat16 [1024, 1024], P('fs', 'sp'), may hold values from -1 to 1
- state_out_weight: bfloat16 [512, 1024], P('fs', 'sp'), may hold values from -0.25 to 0.25
- out_gain: float32 [1024], P('fs'), may hold values from 0.1 to 1.9
Outputs:
- layer_output: bfloat16 [8, 2048, 1024], P('tp', 'sp', 'fs')
The draws below stay inside these ranges and needn't reach their ends.
All inputs are finite; a program needn't handle non-finite values.
Results may differ from the reference program's by a relative error of at most 0.015.
Values may be sent and summed in bfloat16 or wider, within the bound.
A program may use at most 64 MiB of HBM per device.

```python
import math
import jax
import jax.numpy as jnp
from jax import lax

D = 1024
HEAD_DIM = 64
Q_HEADS = 16
KV_HEADS = 4
WINDOW = 128
GROUP = 16
GROUPS = 32
STATE = 64
TOK_DEV = 128
SEQ = 2048
BATCH = 8
Q_WIDTH = 1024
KV_WIDTH = 256
SSM_WIDTH = 512


def level_of(key, extent, cuts, least, top_value):
    factor_of = 1.0
    for axis_at, shards_of in cuts:
        steps = jax.random.uniform(jax.random.fold_in(jax.random.fold_in(key, 6), axis_at), (shards_of,), jnp.float32, least / len(cuts), top_value / len(cuts))
        factor_of = factor_of * jnp.repeat(jnp.exp(steps), extent[axis_at] // shards_of).reshape((-1,) + (1,) * (len(extent) - 1 - axis_at))
    return factor_of


def gaussian(rng, dims, width, reach, split=(), kind=jnp.bfloat16):
    array = width * jax.random.normal(rng, dims, jnp.float32)
    if split:
        array = array * level_of(rng, dims, split, -0.22, 0.18)
    return jnp.clip(array, -reach, reach).astype(kind)


def setup_inputs(seed: int = 0) -> dict:
    key_list = jax.random.split(jax.random.key(seed), 21)
    return {
        "tokens": gaussian(key_list[0], (BATCH, SEQ, D), 1.0, 6.0, ((0, 8), (1, 16))),
        "in_gain": jnp.clip(1.0 + 0.18 * jax.random.normal(key_list[1], (D,), jnp.float32), 0.1, 1.9),
        "query_weight": gaussian(key_list[2], (D, Q_WIDTH), D ** -0.5, 0.1875, ((0, 16), (1, 4))),
        "key_weight": gaussian(key_list[3], (D, KV_WIDTH), D ** -0.5, 0.1875, ((0, 16), (1, 4))),
        "value_weight": gaussian(key_list[4], (D, KV_WIDTH), D ** -0.5, 0.1875, ((0, 16), (1, 4))),
        "attn_gate_weight": gaussian(key_list[5], (D, Q_WIDTH), D ** -0.5, 0.1875, ((0, 16), (1, 4))),
        "state_in_weight": gaussian(key_list[6], (D, SSM_WIDTH), D ** -0.5, 0.1875, ((0, 16), (1, 4))),
        "state_gate_weight": gaussian(key_list[7], (D, SSM_WIDTH), D ** -0.5, 0.1875, ((0, 16), (1, 4))),
        "sink_logits": jnp.clip(2.0 + 4.0 * jax.random.uniform(key_list[8], (Q_HEADS,), jnp.float32) ** level_of(key_list[8], (Q_HEADS,), ((0, 4),), -0.2, 0.2), 2.0, 6.0),
        "decay_rate": jnp.clip(jnp.exp(math.log(1.5) - 3.4011974 * jax.random.uniform(key_list[9], (GROUPS, STATE), jnp.float32) ** level_of(key_list[9], (GROUPS, STATE), ((0, 4),), -0.2, 0.2)), 0.05, 1.5),
        "rotation": jnp.clip(0.3 + 1.2 * jax.random.uniform(key_list[10], (GROUPS, STATE), jnp.float32) ** level_of(key_list[10], (GROUPS, STATE), ((0, 4),), -0.2, 0.2), 0.3, 1.5),
        "step_size": jnp.clip(jnp.exp(math.log(2.0) - 1.3862944 * jax.random.uniform(key_list[11], (GROUPS,), jnp.float32) ** level_of(key_list[11], (GROUPS,), ((0, 4),), -0.2, 0.2)), 0.5, 2.0),
        "input_real": gaussian(key_list[12], (GROUPS, STATE, GROUP), (2 * GROUP) ** -0.5, 1.0, ((0, 4),), jnp.float32),
        "input_imag": gaussian(key_list[13], (GROUPS, STATE, GROUP), (2 * GROUP) ** -0.5, 1.0, ((0, 4),), jnp.float32),
        "output_real": gaussian(key_list[14], (GROUPS, GROUP, STATE), (2 * STATE * SEQ) ** -0.5, 0.01171875, ((0, 4),), jnp.float32),
        "output_imag": gaussian(key_list[15], (GROUPS, GROUP, STATE), (2 * STATE * SEQ) ** -0.5, 0.01171875, ((0, 4),), jnp.float32),
        "skip_scale": gaussian(key_list[16], (SSM_WIDTH,), 1.0, 4.0, ((0, 4),), jnp.float32),
        "focus_result_coefficients": gaussian(key_list[17], (Q_WIDTH, D), (Q_WIDTH // 32) ** -0.5, 1.0, ((0, 4), (1, 16))),
        "state_out_weight": gaussian(key_list[18], (SSM_WIDTH, D), SSM_WIDTH ** -0.5, 0.25, ((0, 4), (1, 16))),
        "out_gain": jnp.clip(1.0 + 0.18 * jax.random.normal(key_list[19], (D,), jnp.float32), 0.1, 1.9),
    }


epsilon = 1e-05
theta_base = 10000.0

def layer_norm(values, gain):
    center = lax.optimization_barrier(jnp.mean(values, axis=-1, keepdims=True))
    spread = lax.optimization_barrier(jnp.mean(jnp.square(values - center), axis=-1, keepdims=True))
    return (values - center) * lax.rsqrt(spread + epsilon) * gain

def rotate(values, positions):
    half = HEAD_DIM // 2
    inv_freq = jnp.power(theta_base, -jnp.arange(half, dtype=jnp.float32) / half)
    angles = positions.astype(jnp.float32)[:, None] * inv_freq
    cosine = jnp.cos(angles)[:, None, :]
    sine = jnp.sin(angles)[:, None, :]
    first = values[..., :half].astype(jnp.float32)
    second = values[..., half:].astype(jnp.float32)
    turned = jnp.concatenate([first * cosine - second * sine, second * cosine + first * sine], axis=-1)
    return turned.astype(jnp.bfloat16)

def discretize(decay_rate, rotation, step_size, input_real, input_imag, sequence_extent):
    real_rate = -decay_rate / sequence_extent
    time_step = step_size[:, None]
    magnitude = jnp.exp(real_rate * time_step)
    decay_real = magnitude * jnp.cos(rotation * time_step)
    decay_imag = magnitude * jnp.sin(rotation * time_step)
    denominator = real_rate * real_rate + rotation * rotation
    factor_real = ((decay_real - 1.0) * real_rate + decay_imag * rotation) / denominator
    factor_imag = (decay_imag * real_rate - (decay_real - 1.0) * rotation) / denominator
    drive_real = factor_real[..., None] * input_real - factor_imag[..., None] * input_imag
    drive_imag = factor_real[..., None] * input_imag + factor_imag[..., None] * input_real
    return (decay_real, decay_imag, drive_real, drive_imag)

def window_attention(queries, key_rows, value_rows, sink_logits):
    batch_count, sequence_extent = (queries.shape[0], queries.shape[1])
    per_group = Q_HEADS // KV_HEADS
    padded_keys = jnp.pad(key_rows, ((0, 0), (WINDOW, 0), (0, 0), (0, 0)))
    padded_values = jnp.pad(value_rows, ((0, 0), (WINDOW, 0), (0, 0), (0, 0)))
    block_count = sequence_extent // TOK_DEV
    sink = sink_logits.reshape(KV_HEADS, per_group)[None, :, :, None, None]

    def one_block(index):
        start = index * TOK_DEV
        grouped = lax.dynamic_slice_in_dim(queries, start, TOK_DEV, 1).astype(jnp.float32)
        grouped = grouped.reshape(batch_count, TOK_DEV, KV_HEADS, per_group, HEAD_DIM)
        near_keys = lax.dynamic_slice_in_dim(padded_keys, start, TOK_DEV + WINDOW, 1).astype(jnp.float32)
        near_values = lax.dynamic_slice_in_dim(padded_values, start, TOK_DEV + WINDOW, 1).astype(jnp.float32)
        scores = jnp.einsum('bqkrd,bckd->bkrqc', grouped, near_keys) * HEAD_DIM ** (-0.5)
        query_pos = start + jnp.arange(TOK_DEV, dtype=jnp.int32)
        key_pos = start - WINDOW + jnp.arange(TOK_DEV + WINDOW, dtype=jnp.int32)
        differ = query_pos[:, None] - key_pos[None, :]
        allowed = (differ >= 0) & (differ < WINDOW) & (key_pos >= 0)[None, :]
        scores = jnp.where(allowed[None, None, None], scores, -jnp.inf)
        largest = jnp.maximum(lax.optimization_barrier(jnp.max(scores, axis=-1, keepdims=True)), sink)
        weights = jnp.exp(scores - largest)
        weights = weights / (lax.optimization_barrier(jnp.sum(weights, axis=-1, keepdims=True)) + jnp.exp(sink - largest))
        rounded = lax.optimization_barrier(weights.astype(jnp.bfloat16))
        attended = jnp.einsum('bkrqc,bckd->bqkrd', rounded.astype(jnp.float32), near_values)
        return attended.reshape(batch_count, TOK_DEV, Q_WIDTH)
    blocks = lax.map(one_block, jnp.arange(block_count, dtype=jnp.int32))
    return jnp.transpose(blocks, (1, 0, 2, 3)).reshape(batch_count, sequence_extent, Q_WIDTH)

def reference(tokens, in_gain, query_weight, key_weight, value_weight, attn_gate_weight, state_in_weight, state_gate_weight, sink_logits, decay_rate, rotation, step_size, input_real, input_imag, output_real, output_imag, skip_scale, focus_result_coefficients, state_out_weight, out_gain):
    batch_count, sequence_extent = (tokens.shape[0], tokens.shape[1])
    highest = lax.Precision.HIGHEST
    normed = layer_norm(tokens.astype(jnp.float32), in_gain).astype(jnp.bfloat16)
    flat_rows = normed.reshape(batch_count * sequence_extent, D)

    def project(number_grid):
        result = jnp.dot(flat_rows, number_grid, preferred_element_type=jnp.float32).astype(jnp.bfloat16)
        return result.reshape(batch_count, sequence_extent, number_grid.shape[1])
    positions = jnp.arange(sequence_extent, dtype=jnp.int32)
    queries = rotate(project(query_weight).reshape(batch_count, sequence_extent, Q_HEADS, HEAD_DIM), positions)
    key_rows = rotate(project(key_weight).reshape(batch_count, sequence_extent, KV_HEADS, HEAD_DIM), positions)
    value_rows = project(value_weight).reshape(batch_count, sequence_extent, KV_HEADS, HEAD_DIM)
    attn_gate = project(attn_gate_weight)
    state_input = project(state_in_weight)
    state_gate = project(state_gate_weight)
    attended = window_attention(queries, key_rows, value_rows, sink_logits)
    gated_attn = (jax.nn.sigmoid(attn_gate.astype(jnp.float32)) * attended).astype(jnp.bfloat16)
    decay_real, decay_imag, drive_real, drive_imag = discretize(decay_rate, rotation, step_size, input_real, input_imag, SEQ)
    inputs_float = state_input.astype(jnp.float32).reshape(batch_count, sequence_extent, GROUPS, GROUP)
    push_real = jnp.einsum('bsgh,gph->sbgp', inputs_float, drive_real, precision=highest)
    push_imag = jnp.einsum('bsgh,gph->sbgp', inputs_float, drive_imag, precision=highest)

    def advance(carry, pushes):
        state_real, state_imag = carry
        new_real = decay_real * state_real - decay_imag * state_imag + pushes[0]
        new_imag = decay_real * state_imag + decay_imag * state_real + pushes[1]
        return ((new_real, new_imag), (new_real, new_imag))
    nothing_values = jnp.zeros((batch_count, GROUPS, STATE), jnp.float32)
    _, (all_real, all_imag) = lax.scan(advance, (nothing_values, nothing_values), (push_real, push_imag))
    final_reading = jnp.einsum('sbgp,ghp->bsgh', all_real, output_real, precision=highest) - jnp.einsum('sbgp,ghp->bsgh', all_imag, output_imag, precision=highest)
    final_reading = final_reading + skip_scale.reshape(GROUPS, GROUP) * inputs_float
    final_reading = final_reading.reshape(batch_count, sequence_extent, SSM_WIDTH)
    gated_state = (jax.nn.gelu(final_reading, approximate=False) * jax.nn.sigmoid(state_gate.astype(jnp.float32))).astype(jnp.bfloat16)
    mixed = jnp.dot(gated_attn.reshape(-1, Q_WIDTH), focus_result_coefficients, preferred_element_type=jnp.float32) + jnp.dot(gated_state.reshape(-1, SSM_WIDTH), state_out_weight, preferred_element_type=jnp.float32)
    result = layer_norm(mixed, out_gain).astype(jnp.bfloat16)
    return result.reshape(batch_count, sequence_extent, D)
```

```python
import functools
import math

import jax
import jax.numpy as jnp
from jax import lax
from jax.experimental import pallas as pl
from jax.experimental.pallas import tpu as pltpu
from jax.sharding import PartitionSpec as P

HEAD_DIM = 64
GROUP = 16
STATE = 64
EPS = 1e-05
THETA = 10000.0
CHUNKS = 4

F32 = jnp.float32
BF16 = jnp.bfloat16
MESH = pl.DeviceIdType.MESH


def nn(a, b, precision=None):
    return lax.dot_general(
        a, b, (((1,), (0,)), ((), ())), precision=precision, preferred_element_type=F32
    )


def nt(a, b, precision=None):
    return lax.dot_general(
        a, b, (((1,), (1,)), ((), ())), precision=precision, preferred_element_type=F32
    )


def cmul(ar, ai, br, bi):
    return ar * br - ai * bi, ar * bi + ai * br


def kernel(
    sp_n, fs_n,
    tok, gain, wq, wk, wv, wg, wsi, wsg, sink, decay, rot, step, inr, ini, outr, outi,
    skip, wf, wso, ogain,
    out,
    W, normed, prow, Er, Ei, DM, CM, PW, cos_t, sin_t, Hr, Hi,
    kv_own, kv_prev, q_s, gate_s, sgate_s, u_s, att_s,
    s_own, s_in, mix_s, rs_out, rs_in, st_out, st_in,
    z_send, z_recv, c_send, c_recv, kv_send, kv_recv, s_send, s_recv,
    rs_send, rs_recv, st_send, st_recv,
):
    z = lax.axis_index("sp")
    y = lax.axis_index("fs")
    tp = lax.axis_index("tp")
    c = lax.rem(tp, 2)
    mate = tp + 1 - 2 * c
    up = lax.rem(z + 1, sp_n)
    down = lax.rem(z + sp_n - 1, sp_n)
    rows = wq.shape[0]
    tokens = tok.shape[1]
    piece = rows // CHUNKS
    n_up = sp_n // 2
    n_down = sp_n - 1 - n_up

    barrier = pltpu.get_barrier_semaphore()
    pl.semaphore_signal(barrier, inc=1, device_id={"sp": up}, device_id_type=MESH)
    pl.semaphore_signal(barrier, inc=1, device_id={"sp": down}, device_id_type=MESH)
    pl.semaphore_signal(barrier, inc=1, device_id={"tp": mate}, device_id_type=MESH)
    for d in range(1, fs_n):
        pl.semaphore_signal(
            barrier, inc=1, device_id={"fs": lax.rem(y + d, fs_n)}, device_id_type=MESH
        )

    own = pl.ds(pl.multiple_of(z * rows, rows), rows)
    W[0, own, 0:128] = wsi[...]
    W[0, own, 128:192] = wk[...]
    W[0, own, 192:256] = wv[...]
    W[0, own, 256:384] = wsg[...]
    W[0, own, 384:640] = wq[...]
    W[1, own, 0:256] = wg[...]
    eye = (
        lax.broadcasted_iota(jnp.int32, (rows, rows), 0)
        == lax.broadcasted_iota(jnp.int32, (rows, rows), 1)
    ).astype(BF16)
    W[1, own, 256:512] = nt(eye, wf[...]).astype(BF16)
    W[1, own, 512:640] = nt(eye, wso[...]).astype(BF16)

    pl.semaphore_wait(barrier, 3 + fs_n - 1)

    def shard(direction, k):
        return lax.rem(z + sp_n - k, sp_n) if direction == 0 else lax.rem(z + k, sp_n)

    def z_copy(direction, k, i):
        at = pl.multiple_of(shard(direction, k) * rows + i * piece, piece)
        ref = W.at[c, pl.ds(at, piece), :]
        return pltpu.make_async_remote_copy(
            src_ref=ref, dst_ref=ref,
            send_sem=z_send.at[direction], recv_sem=z_recv.at[direction, k, i],
            device_id={"sp": up if direction == 0 else down}, device_id_type=MESH,
        )

    def z_arrival(direction, k, i):
        at = pl.multiple_of(shard(direction, k + 1) * rows + i * piece, piece)
        ref = W.at[c, pl.ds(at, piece), :]
        return pltpu.make_async_remote_copy(
            src_ref=ref, dst_ref=ref,
            send_sem=z_send.at[direction], recv_sem=z_recv.at[direction, k, i],
            device_id={"sp": up if direction == 0 else down}, device_id_type=MESH,
        )

    def c_copy(direction, k):
        at = pl.multiple_of(shard(direction, k) * rows, rows)
        ref = W.at[c, pl.ds(at, rows), :]
        return pltpu.make_async_remote_copy(
            src_ref=ref, dst_ref=ref, send_sem=c_send, recv_sem=c_recv,
            device_id={"tp": mate}, device_id_type=MESH,
        )

    for i in range(CHUNKS):
        z_copy(0, 0, i).start()
        z_copy(1, 0, i).start()

    def work_norm(lo, hi):
        x = tok[0, lo:hi, :].astype(F32)
        width = x.shape[-1]
        center = jnp.sum(x, axis=-1, keepdims=True) / width
        x = x - center
        spread = jnp.sum(x * x, axis=-1, keepdims=True) / width
        normed[lo:hi, :] = (x * lax.rsqrt(spread + EPS) * gain[...]).astype(BF16)

    def work_rope():
        lane = lax.broadcasted_iota(jnp.int32, (1, 128), 1)
        inv = jnp.exp(lax.rem(lane, 32).astype(F32) * (-2.0 * math.log(THETA) / HEAD_DIM))
        r1, i1 = jnp.cos(inv), jnp.sin(inv)
        sub = lax.broadcasted_iota(jnp.int32, (8, 128), 0)
        br = jnp.ones((8, 128), F32)
        bi = jnp.zeros((8, 128), F32)
        pr, pi = jnp.ones((1, 128), F32), jnp.zeros((1, 128), F32)
        for r in range(1, 8):
            pr, pi = cmul(pr, pi, r1, i1)
            br = jnp.where(sub == r, pr, br)
            bi = jnp.where(sub == r, pi, bi)
        sr, si = cmul(pr, pi, r1, i1)
        full_r, full_i = br, bi
        while full_r.shape[0] < tokens:
            nr, ni = cmul(full_r, full_i, sr, si)
            full_r = jnp.concatenate([full_r, nr], axis=0)
            full_i = jnp.concatenate([full_i, ni], axis=0)
            sr, si = cmul(sr, si, sr, si)
        zr, zi = jnp.ones((1, 128), F32), jnp.zeros((1, 128), F32)
        bit = 1
        while bit < sp_n:
            on = jnp.full((1, 128), lax.rem(z // bit, 2), jnp.int32) == 1
            nr, ni = cmul(zr, zi, sr, si)
            zr = jnp.where(on, nr, zr)
            zi = jnp.where(on, ni, zi)
            sr, si = cmul(sr, si, sr, si)
            bit *= 2
        full_r, full_i = cmul(full_r, full_i, zr, zi)
        first = lax.rem(lax.broadcasted_iota(jnp.int32, (tokens, 128), 1), 64) < 32
        cos_t[...] = full_r
        sin_t[...] = jnp.where(first, -full_i, full_i)

    def work_rows():
        for g in range(8):
            at = slice(STATE * g, STATE * g + STATE)
            prow[0:1, at] = decay[g : g + 1, :]
            prow[1:2, at] = rot[g : g + 1, :]
            prow[2:3, at] = jnp.full((1, STATE), step[g], F32)

    def work_states():
        rate = -prow[0:1, :] / float(sp_n * tokens)
        turn = prow[1:2, :]
        dt = prow[2:3, :]
        size = jnp.exp(rate * dt)
        ar, ai = size * jnp.cos(turn * dt), size * jnp.sin(turn * dt)
        den = rate * rate + turn * turn
        prow[3:4, :] = ((ar - 1.0) * rate + ai * turn) / den
        prow[4:5, :] = (ai * rate - (ar - 1.0) * turn) / den
        sub = lax.broadcasted_iota(jnp.int32, (8, 512), 0)
        br = jnp.broadcast_to(ar, (8, 512))
        bi = jnp.broadcast_to(ai, (8, 512))
        pr, pi = ar, ai
        for r in range(1, 8):
            pr, pi = cmul(pr, pi, ar, ai)
            br = jnp.where(sub == r, pr, br)
            bi = jnp.where(sub == r, pi, bi)
        Er[0:8, :] = br
        Ei[0:8, :] = bi
        sr, si = pr, pi
        n = 8
        while n < tokens:
            nr, ni = cmul(Er[0:n, :], Ei[0:n, :], sr, si)
            Er[n : 2 * n, :] = nr
            Ei[n : 2 * n, :] = ni
            sr, si = cmul(sr, si, sr, si)
            n *= 2
        pr, pi = jnp.ones((1, 512), F32), jnp.zeros((1, 512), F32)
        for d in range(sp_n):
            PW[d, :, 0:512] = pr
            PW[d, :, 512:1024] = pi
            pr, pi = cmul(pr, pi, sr, si)

    def work_drive():
        pick = (
            lax.rem(lax.broadcasted_iota(jnp.int32, (128, GROUP), 0), GROUP)
            == lax.broadcasted_iota(jnp.int32, (128, GROUP), 1)
        ).astype(F32)
        high = lax.Precision.HIGHEST
        xr = nt(pick, inr[...].reshape(8 * STATE, GROUP), high)
        xi = nt(pick, ini[...].reshape(8 * STATE, GROUP), high)
        fr, fi = prow[3:4, :], prow[4:5, :]
        dr, di = cmul(fr, fi, xr, xi)
        same = (
            lax.broadcasted_iota(jnp.int32, (128, 512), 0) // GROUP
            == lax.broadcasted_iota(jnp.int32, (128, 512), 1) // STATE
        )
        DM[:, 0:512] = jnp.where(same, dr, 0.0).astype(BF16)
        DM[:, 512:1024] = jnp.where(same, di, 0.0).astype(BF16)

    def work_read():
        pick = (
            lax.rem(lax.broadcasted_iota(jnp.int32, (STATE, 512), 1), STATE)
            == lax.broadcasted_iota(jnp.int32, (STATE, 512), 0)
        ).astype(BF16)
        same = (
            lax.broadcasted_iota(jnp.int32, (128, 512), 0) // GROUP
            == lax.broadcasted_iota(jnp.int32, (128, 512), 1) // STATE
        )
        cr = nn(outr[...].reshape(128, STATE).astype(BF16), pick)
        ci = nn(outi[...].reshape(128, STATE).astype(BF16), pick)
        CM[:, 0:512] = jnp.where(same, cr, 0.0).astype(BF16)
        CM[:, 512:1024] = jnp.where(same, -ci, 0.0).astype(BF16)

    half = tokens // 2
    work = [
        functools.partial(work_norm, 0, half),
        functools.partial(work_norm, half, tokens),
        work_rope,
        work_rows,
        work_states,
        work_drive,
        work_read,
    ]
    for k in range(n_up):
        if k < len(work):
            work[k]()
        for i in range(CHUNKS):
            z_arrival(0, k, i).wait_recv()
            if k + 1 < n_up:
                z_copy(0, k + 1, i).start()
            if k < n_down:
                z_arrival(1, k, i).wait_recv()
                if k + 1 < n_down:
                    z_copy(1, k + 1, i).start()
        c_copy(0, k + 1).start()
        if k < n_down:
            c_copy(1, k + 1).start()
    others = pl.ds(0, (sp_n - 1) * rows)

    def c_total(h):
        ref = W.at[h, others, :]
        return pltpu.make_async_remote_copy(
            src_ref=ref, dst_ref=ref, send_sem=c_send, recv_sem=c_recv,
            device_id={"tp": mate}, device_id_type=MESH,
        )

    c_total(1 - c).wait_recv()

    lane128 = lax.broadcasted_iota(jnp.int32, (tokens, 128), 1)
    first = lax.rem(lane128, 64) < 32

    def turned(v, co, si):
        swapped = jnp.where(first, pltpu.roll(v, 96, 1), pltpu.roll(v, 32, 1))
        return v * co + swapped * si

    uk = nn(normed[...], W[0, :, 0:256])
    u = uk[:, 0:128].astype(BF16)
    kv = uk[:, 128:256].astype(BF16).astype(F32)
    key_part = lane128 < 64
    kv_own[...] = jnp.where(key_part, turned(kv, cos_t[...], sin_t[...]), kv).astype(BF16)
    u_s[...] = u
    kv_copy = pltpu.make_async_remote_copy(
        src_ref=kv_own, dst_ref=kv_prev, send_sem=kv_send, recv_sem=kv_recv,
        device_id={"sp": up}, device_id_type=MESH,
    )

    def shifted(v, n, sub):
        if n % 8 == 0:
            return jnp.concatenate([jnp.zeros((n, v.shape[1]), F32), v[: tokens - n, :]], axis=0)
        return jnp.where(sub >= n, pltpu.roll(v, n, 0), 0.0)

    sub128 = lax.broadcasted_iota(jnp.int32, (tokens, 128), 0)
    for b in range(4):
        at = slice(128 * b, 128 * b + 128)
        hr = nn(u, DM[:, at])
        hi = nn(u, DM[:, slice(512 + 128 * b, 640 + 128 * b)])
        n = 1
        while n < tokens:
            ar, ai = Er[n - 1 : n, at], Ei[n - 1 : n, at]
            mr, mi = cmul(ar, ai, shifted(hr, n, sub128), shifted(hi, n, sub128))
            hr, hi = hr + mr, hi + mi
            n *= 2
        Hr[:, at] = hr
        Hi[:, at] = hi
        s_own[:, at] = hr[tokens - 1 : tokens, :]
        s_own[:, slice(512 + 128 * b, 640 + 128 * b)] = hi[tokens - 1 : tokens, :]
    kv_copy.start()

    def s_copy(d):
        return pltpu.make_async_remote_copy(
            src_ref=s_own, dst_ref=s_in.at[d], send_sem=s_send.at[d], recv_sem=s_recv.at[d],
            device_id={"sp": lax.rem(z + d, sp_n)}, device_id_type=MESH,
        )

    qg = nn(normed[...], W[0, :, 256:640])
    for d in range(1, sp_n):
        @pl.when(z + d < sp_n)
        def _(d=d):
            s_copy(d).start()
    sgate_s[...] = jax.nn.sigmoid(qg[:, 0:128].astype(BF16).astype(F32))
    for b in range(2):
        raw = qg[:, 128 + 128 * b : 256 + 128 * b].astype(BF16).astype(F32)
        q_s[:, 128 * b : 128 * b + 128] = turned(raw, cos_t[...], sin_t[...]).astype(BF16)
    gate_s[...] = jax.nn.sigmoid(nn(normed[...], W[1, :, 0:256]).astype(BF16).astype(F32))

    kv_copy.wait_recv()
    mine = kv_own[...].astype(F32)
    past = kv_prev[...].astype(F32)
    low = lane128 < 64
    zero = jnp.zeros_like(mine)

    def sides(v):
        turned_v = pltpu.roll(v, 64, 1)
        keys = [jnp.where(low, v, zero).astype(BF16), jnp.where(low, zero, turned_v).astype(BF16)]
        vals = [jnp.where(low, turned_v, zero).astype(BF16), jnp.where(low, zero, v).astype(BF16)]
        return keys, vals

    mine_k, mine_v = sides(mine)
    past_k, past_v = sides(past)
    lower = lax.broadcasted_iota(jnp.int32, (tokens, tokens), 1) <= lax.broadcasted_iota(
        jnp.int32, (tokens, tokens), 0
    )
    has_past = jnp.full((tokens, tokens), z, jnp.int32) > 0
    for b in range(2):
        qb = q_s[:, 128 * b : 128 * b + 128]
        total = None
        for s in range(2):
            sc = jnp.where(lower, nt(qb, mine_k[s]), nt(qb, past_k[s])) * (HEAD_DIM ** -0.5)
            sc = jnp.where(lower | has_past, sc, -1e30)
            logit = sink[2 * b + s]
            top = jnp.maximum(jnp.max(sc, axis=-1, keepdims=True), logit)
            w = jnp.exp(sc - top)
            w = w / (jnp.sum(w, axis=-1, keepdims=True) + jnp.exp(logit - top))
            wz = jnp.zeros_like(w)
            part = nn(jnp.where(lower, w, wz).astype(BF16), mine_v[s])
            part = part + nn(jnp.where(lower, wz, w).astype(BF16), past_v[s])
            total = part if total is None else total + part
        at = slice(128 * b, 128 * b + 128)
        att_s[:, at] = (gate_s[:, at] * total).astype(BF16)

    mix_s[...] = nt(att_s[...], W[1, :, 256:512])

    cr = jnp.zeros((1, 512), F32)
    ci = jnp.zeros((1, 512), F32)
    for d in range(1, sp_n):
        @pl.when(z >= d)
        def _(d=d):
            s_copy(d).wait_recv()
        on = jnp.full((1, 512), z, jnp.int32) >= d
        tr, ti = cmul(
            PW[d - 1, :, 0:512], PW[d - 1, :, 512:1024], s_in[d, :, 0:512], s_in[d, :, 512:1024]
        )
        cr = cr + jnp.where(on, tr, 0.0)
        ci = ci + jnp.where(on, ti, 0.0)
    fr, fi = cmul(Er[...], Ei[...], cr, ci)
    reading = nt((Hr[...] + fr).astype(BF16), CM[:, 0:512])
    reading = reading + nt((Hi[...] + fi).astype(BF16), CM[:, 512:1024])
    reading = reading + skip[...] * u_s[...].astype(F32)
    gelu = 0.5 * reading * (1.0 + lax.erf(reading * math.sqrt(0.5)))
    gated_state = (gelu * sgate_s[...]).astype(BF16)

    width = mix_s.shape[1]
    feats = width // fs_n

    def rs_copy(d):
        return pltpu.make_async_remote_copy(
            src_ref=rs_out.at[d], dst_ref=rs_in.at[d],
            send_sem=rs_send.at[d], recv_sem=rs_recv.at[d],
            device_id={"fs": lax.rem(y + d, fs_n)}, device_id_type=MESH,
        )

    def features(d):
        at = pl.ds(pl.multiple_of(lax.rem(y + d, fs_n) * feats, feats), feats)
        return mix_s[:, at] + nt(gated_state, W[1, at, 512:640])

    order = [fs_n // 2] + [d for d in range(1, fs_n) if d != fs_n // 2]
    for d in order:
        rs_out[d] = features(d).astype(BF16)
    for d in order:
        rs_copy(d).start()
    mixed = features(0)
    for d in order[1:] + order[:1]:
        rs_copy(d).wait_recv()
        mixed = mixed + rs_in[d].astype(F32)

    mean = jnp.sum(mixed, axis=-1, keepdims=True) / feats
    dev = mixed - mean
    sq = jnp.sum(dev * dev, axis=-1, keepdims=True)
    tile = jnp.where(lane128 == 0, mean, jnp.where(lane128 == 1, sq, 0.0))
    st_out[...] = jnp.transpose(tile)[0:8, :]

    def st_copy(d):
        return pltpu.make_async_remote_copy(
            src_ref=st_out, dst_ref=st_in.at[d],
            send_sem=st_send.at[d], recv_sem=st_recv.at[d],
            device_id={"fs": lax.rem(y + d, fs_n)}, device_id_type=MESH,
        )

    for d in order:
        st_copy(d).start()
    tiles = [st_out[...]]
    for d in order[1:] + order[:1]:
        st_copy(d).wait_recv()
        tiles.append(st_in[d])
    mean_row = sum(t[0:1, :] for t in tiles) / fs_n
    sq_row = sum(t[1:2, :] + feats * jnp.square(t[0:1, :] - mean_row) for t in tiles)
    scale_row = lax.rsqrt(sq_row / width + EPS)
    sub_sq = lax.broadcasted_iota(jnp.int32, (128, 128), 0)
    both = jnp.where(sub_sq == 0, mean_row, jnp.where(sub_sq == 1, scale_row, 0.0))
    both = jnp.transpose(both)
    out[0] = ((mixed - both[:, 0:1]) * both[:, 1:2] * ogain[...]).astype(BF16)

    for direction, steps in ((0, n_up), (1, n_down)):
        ref = W.at[0, pl.ds(0, steps * rows), :]
        pltpu.make_async_remote_copy(
            src_ref=ref, dst_ref=ref,
            send_sem=z_send.at[direction], recv_sem=z_recv.at[direction, 0, 0],
            device_id={"sp": up}, device_id_type=MESH,
        ).wait_send()
    c_total(0).wait_send()
    kv_copy.wait_send()
    for d in range(1, sp_n):
        @pl.when(z + d < sp_n)
        def _(d=d):
            s_copy(d).wait_send()
    for d in order:
        rs_copy(d).wait_send()
        st_copy(d).wait_send()


def local(sp_n, fs_n, *args):
    (
        tokens, in_gain, query, key, value, attn_gate, state_in, state_gate, sink, decay, rotation,
        step, in_r, in_i, out_r, out_i, skip, focus, state_out, out_gain,
    ) = args
    t = tokens.shape[1]
    rows = query.shape[0]
    width = tokens.shape[2]
    feats = width // fs_n
    vm = pl.BlockSpec(memory_space=pltpu.VMEM)
    sm = pl.BlockSpec(memory_space=pltpu.SMEM)
    specs = [vm] * 8 + [sm, vm, vm, sm] + [vm] * 8
    n_up = sp_n // 2
    V, dma = pltpu.VMEM, pltpu.SemaphoreType.DMA
    return pl.pallas_call(
        functools.partial(kernel, sp_n, fs_n),
        out_shape=jax.ShapeDtypeStruct((1, t, feats), BF16),
        in_specs=specs,
        out_specs=vm,
        scratch_shapes=[
            V((2, sp_n * rows, 640), BF16), V((t, width), BF16), V((8, 512), F32),
            V((t, 512), F32), V((t, 512), F32), V((128, 1024), BF16), V((128, 1024), BF16),
            V((sp_n, 1, 1024), F32), V((t, 128), F32), V((t, 128), F32),
            V((t, 512), F32), V((t, 512), F32),
            V((t, 128), BF16), V((t, 128), BF16), V((t, 256), BF16), V((t, 256), F32),
            V((t, 128), F32), V((t, 128), BF16), V((t, 256), BF16),
            V((1, 1024), F32), V((sp_n, 1, 1024), F32), V((t, width), F32),
            V((fs_n, t, feats), BF16), V((fs_n, t, feats), BF16),
            V((8, 128), F32), V((fs_n, 8, 128), F32),
            dma((2,)), dma((2, n_up, CHUNKS)), dma, dma, dma, dma, dma((sp_n,)), dma((sp_n,)),
            dma((fs_n,)), dma((fs_n,)), dma((fs_n,)), dma((fs_n,)),
        ],
        compiler_params=pltpu.CompilerParams(
            collective_id=0, has_side_effects=True, vmem_limit_bytes=48 * 1024 * 1024
        ),
        name="layer",
    )(
        tokens, in_gain.reshape(1, -1), query, key, value, attn_gate, state_in, state_gate, sink,
        decay, rotation, step, in_r, in_i, out_r, out_i, skip.reshape(1, -1), focus, state_out,
        out_gain.reshape(1, -1),
    )


def solution(mesh):
    sizes = dict(mesh.shape)
    return jax.shard_map(
        functools.partial(local, sizes["sp"], sizes["fs"]),
        mesh=mesh,
        in_specs=(
            P("tp", "sp", None),
            P(),
            P("sp", "fs"),
            P("sp", "fs"),
            P("sp", "fs"),
            P("sp", "fs"),
            P("sp", "fs"),
            P("sp", "fs"),
            P("fs"),
            P("fs", None),
            P("fs", None),
            P("fs"),
            P("fs", None, None),
            P("fs", None, None),
            P("fs", None, None),
            P("fs", None, None),
            P("fs"),
            P("fs", "sp"),
            P("fs", "sp"),
            P("fs"),
        ),
        out_specs=P("tp", "sp", "fs"),
        check_vma=False,
    )
```
